32 devices in a mesh: sp: 8 (over z, y), tp: 4 (over x, core).
Axes of the slice: x: 2, y: 2, z: 4, core: 2. Of those that a mesh axis runs over, the one named last changes fastest.
Arguments:
- residual_entry_input: bfloat16 [8192, 2048], P(('sp', 'tp')), may hold values from -6 to 6
- query_matrix_rows: bfloat16 [8192, 1024], P('sp', 'tp'), may hold values from -6 to 6
- key_matrix_rows: bfloat16 [8192, 1024], P('sp', 'tp'), may hold values from -6 to 6
- value_matrix_rows: bfloat16 [8192, 2048], P('sp', 'tp'), may hold values from -6 to 6
- output_gate_logits: bfloat16 [8192, 2048], P('sp', 'tp'), may hold values from -6 to 6
- input_gate_logits: float32 [8192, 8], P('sp', 'tp'), may hold values from -6 to 6
- forget_gate_logits: float32 [8192, 8], P('sp', 'tp'), may hold values from -8 to 31
- forget_decay_offset: float32 [8192, 8], P('sp', 'tp'), may hold values from -0.7 to 0
- head_norm_gain: float32 [8, 256], P('tp'), may hold values from 0.1 to 1.9
- cell_output_weight: bfloat16 [2048, 2048], P('tp'), may hold values from -0.125 to 0.125
- feedforward_norm_gain: float32 [2048], replicated, may hold values from 0.1 to 1.9
- gate_up_weight: bfloat16 [2048, 5632], P('sp', 'tp'), may hold values from -0.125 to 0.125
- value_up_weight: bfloat16 [2048, 5632], P('sp', 'tp'), may hold values from -0.125 to 0.125
- gate_filter_taps: float32 [3, 5632], P(None, 'tp'), may hold values from -3 to 3
- value_filter_taps: float32 [3, 5632], P(None, 'tp'), may hold values from -3 to 3
- down_projection_weight: bfloat16 [5632, 2048], P('tp', 'sp'), may hold values from -0.078125 to 0.078125
Outputs:
- result: bfloat16 [8192, 2048], P(('sp', 'tp'))
The draws below stay inside these ranges and needn't reach their ends.
All inputs are finite; a program needn't handle non-finite values.
Results may differ from the reference program's by a relative error of at most 0.025.
Values may be sent and summed in bfloat16 or wider, within the bound.
No kernel may reach another device: no remote copies, remote signals or barrier semaphores. Data moves between devices by JAX's collectives and lax.ppermute only.
A program may use at most 128 MiB of HBM per device.

```python
import math
import jax
import jax.numpy as jnp
from jax import lax

D = 2048
HEADS = 8
DK = 128
DV = 256
FF = 5632
BLOCK = 128
TOK_DEV = 1024
TOKENS = 8192
HV = 2048
FF_DEV = 1408
N_TP = 4


def draw_forget_gate_logits(key, part):
    key_order = jax.random.fold_in(key, 11)
    key_slow = jax.random.fold_in(key, 12)
    key_fast = jax.random.fold_in(key, 13)
    key_noise = jax.random.fold_in(key, 14)
    order = jax.random.permutation(key_order, HEADS)
    slow_heads = order < HEADS // 2
    slow_rate = math.log(10.0) / (6.0 * TOKENS) * jnp.exp(jax.random.uniform(key_slow, (HEADS,), jnp.float32, math.log(0.5), 0.0))
    fast_rate = 1.0 / 40.0 * jnp.exp(jax.random.uniform(key_fast, (HEADS,), jnp.float32, math.log(0.6), math.log(1.6)))
    head_rate = jnp.where(slow_heads, slow_rate, fast_rate)
    block_index = jnp.arange(TOKENS) // TOK_DEV
    device_factor = (1 + block_index % 2).astype(jnp.float32)
    noise = jnp.clip(jax.random.normal(key_noise, (TOKENS, HEADS), jnp.float32), -4.0, 4.0)
    rate = head_rate[None, :] * device_factor[:, None] * jnp.exp(0.7 * noise)
    capped = jnp.clip(-jnp.log(jnp.expm1(rate)), -6.0, 14.5)
    ratio = capped / 15.0
    return (7.5 * jnp.log((1.0 + ratio) / (1.0 - ratio))).astype(jnp.float32)


def draw_forget_decay_offset(key, part):
    key_where = jax.random.fold_in(key, 21)
    key_depth = jax.random.fold_in(key, 22)
    spots = jax.random.randint(key_where, (2,), 0, TOKENS)
    depth = jax.random.uniform(key_depth, (2, HEADS), jnp.float32, math.log(0.5), math.log(0.8))
    positions = jnp.arange(TOKENS)
    first = jnp.where((positions == spots[0])[:, None], depth[0][None, :], 0.0)
    second = jnp.where((positions == spots[1])[:, None], depth[1][None, :], 0.0)
    return (first + second).astype(jnp.float32)


def steps_of(rng, extent, split, low, top_value):
    def one(axis_at, blocks):
        draws = jax.random.uniform(jax.random.fold_in(jax.random.fold_in(rng, 6), axis_at), (blocks,), jnp.float32, low / len(split), top_value / len(split))
        return jnp.repeat(jnp.exp(draws), extent[axis_at] // blocks).reshape((-1,) + (1,) * (len(extent) - axis_at - 1))

    factor_of = one(*split[0])
    for cut in split[1:]:
        factor_of = factor_of * one(*cut)
    return factor_of


def normal_values(own_key, dims, width, most, cuts=(), kind=jnp.bfloat16):
    array = width * jax.random.normal(own_key, dims, jnp.float32)
    if cuts:
        array = array * steps_of(own_key, dims, cuts, -0.22, 0.18)
    return jnp.clip(array, -most, most).astype(kind)


def setup_inputs(seed: int = 0) -> dict:
    keys = jax.random.split(jax.random.key(seed), 17)
    return {
        "residual_entry_input": normal_values(keys[0], (TOKENS, D), 1.0, 6.0, ((0, 32),)),
        "query_matrix_rows": normal_values(keys[1], (TOKENS, HEADS * DK), 1.0, 6.0, ((0, 8), (1, 4))),
        "key_matrix_rows": normal_values(keys[2], (TOKENS, HEADS * DK), 1.0, 6.0, ((0, 8), (1, 4))),
        "value_matrix_rows": normal_values(keys[3], (TOKENS, HV), 1.0, 6.0, ((0, 8), (1, 4))),
        "output_gate_logits": normal_values(keys[4], (TOKENS, HV), 1.0, 6.0, ((0, 8), (1, 4))),
        "input_gate_logits": normal_values(keys[5], (TOKENS, HEADS), 1.0, 6.0, ((0, 8), (1, 4)), jnp.float32),
        "forget_gate_logits": draw_forget_gate_logits(jax.random.fold_in(keys[16], 71), 0),
        "forget_decay_offset": draw_forget_decay_offset(jax.random.fold_in(keys[16], 71), 0),
        "head_norm_gain": jnp.clip(1.0 + 0.18 * jax.random.normal(keys[8], (HEADS, DV), jnp.float32), 0.1, 1.9),
        "cell_output_weight": normal_values(keys[9], (HV, D), HV ** -0.5, 0.125, ((0, 4),)),
        "feedforward_norm_gain": jnp.clip(1.0 + 0.18 * jax.random.normal(keys[10], (D,), jnp.float32), 0.1, 1.9),
        "gate_up_weight": normal_values(keys[11], (D, FF), D ** -0.5, 0.125, ((0, 8), (1, 4))),
        "value_up_weight": normal_values(keys[12], (D, FF), D ** -0.5, 0.125, ((0, 8), (1, 4))),
        "gate_filter_taps": normal_values(keys[13], (3, FF), 0.577, 3.0, ((1, 4),), jnp.float32),
        "value_filter_taps": normal_values(keys[14], (3, FF), 0.577, 3.0, ((1, 4),), jnp.float32),
        "down_projection_weight": normal_values(keys[15], (FF, D), FF ** -0.5, 0.078125, ((0, 4), (1, 8))),
    }


eps = 1e-06

def gate_log_values(input_gate_logits, forget_gate_logits, forget_decay_offset):
    input_log_value = 15.0 * jnp.tanh(input_gate_logits / 15.0)
    forget_log_sigmoid = jax.nn.log_sigmoid(15.0 * jnp.tanh(forget_gate_logits / 15.0)) + forget_decay_offset
    return (input_log_value, forget_log_sigmoid)

def block_step(state_carry, inputs):
    memory, normer, running = state_carry
    query_block, key_block, value_block, input_block, forget_block = inputs
    length = query_block.shape[0]
    highest = lax.Precision.HIGHEST
    query_scale = DK ** (-0.5)
    query_wide = query_block.astype(jnp.float32)
    key_wide = key_block.astype(jnp.float32)
    value_wide = value_block.astype(jnp.float32)
    causal = jnp.tril(jnp.ones((length, length), dtype=bool))[:, :, None]
    cumulative = jnp.cumsum(forget_block, axis=0)
    logits = cumulative[:, None, :] - cumulative[None, :, :] + input_block[None, :, :]
    logits = jnp.where(causal, logits, -jnp.inf)
    carried = cumulative + running[None, :]
    stable = jnp.maximum(carried, lax.optimization_barrier(jnp.max(logits, axis=1)))
    carry_weight = jnp.exp(carried - stable)
    raw = jnp.einsum('thd,shd->tsh', query_wide, key_wide) * query_scale
    scores = raw * jnp.exp(logits - stable[:, None, :])
    scores_low = scores.astype(jnp.bfloat16).astype(jnp.float32)
    scaled_query = query_wide * query_scale
    numerator = carry_weight[:, :, None] * jnp.einsum('hvd,thd->thv', memory, scaled_query, precision=highest)
    numerator = numerator + jnp.einsum('tsh,shv->thv', scores_low, value_wide)
    denominator = carry_weight * jnp.einsum('hd,thd->th', normer, scaled_query, precision=highest) + lax.optimization_barrier(jnp.sum(scores, axis=1))
    output = numerator / jnp.maximum(jnp.abs(denominator), jnp.exp(-stable))[:, :, None]
    last_sum = cumulative[-1]
    weights_log = last_sum[None, :] - cumulative + input_block
    new_running = jnp.maximum(last_sum + running, lax.optimization_barrier(jnp.max(weights_log, axis=0)))
    decay_factor = jnp.exp(last_sum + running - new_running)
    weighted = key_wide * jnp.exp(weights_log - new_running[None, :])[:, :, None]
    weighted_low = weighted.astype(jnp.bfloat16).astype(jnp.float32)
    memory = decay_factor[:, None, None] * memory + jnp.einsum('shv,shd->hvd', value_wide, weighted_low)
    normer = decay_factor[:, None] * normer + lax.optimization_barrier(jnp.sum(weighted, axis=0))
    return ((memory, normer, new_running), output)

def reference(residual_entry_input, query_matrix_rows, key_matrix_rows, value_matrix_rows, output_gate_logits, input_gate_logits, forget_gate_logits, forget_decay_offset, head_norm_gain, cell_output_weight, feedforward_norm_gain, gate_up_weight, value_up_weight, gate_filter_taps, value_filter_taps, down_projection_weight):
    token_count = query_matrix_rows.shape[0]
    queries = query_matrix_rows.reshape(token_count, HEADS, DK)
    keys_all = key_matrix_rows.reshape(token_count, HEADS, DK)
    values_all = value_matrix_rows.reshape(token_count, HEADS, DV)
    input_log_value, forget_log_sigmoid = gate_log_values(input_gate_logits, forget_gate_logits, forget_decay_offset)
    block_count = token_count // BLOCK

    def blocks(tensor):
        return tensor.reshape((block_count, BLOCK) + tensor.shape[1:])
    initial = (jnp.zeros((HEADS, DV, DK), jnp.float32), jnp.zeros((HEADS, DK), jnp.float32), jnp.zeros((HEADS,), jnp.float32))
    _, outputs = lax.scan(block_step, initial, (blocks(queries), blocks(keys_all), blocks(values_all), blocks(input_log_value), blocks(forget_log_sigmoid)))
    memory_out = outputs.reshape(token_count, HEADS, DV)
    normed = memory_out * lax.rsqrt(lax.optimization_barrier(jnp.mean(memory_out * memory_out, axis=-1, keepdims=True)) + eps) * head_norm_gain[None, :, :]
    gated_rows = (normed.reshape(token_count, HEADS * DV) * jax.nn.sigmoid(output_gate_logits.astype(jnp.float32))).astype(jnp.bfloat16)
    mixed_rows = jnp.dot(gated_rows, cell_output_weight, preferred_element_type=jnp.float32)
    stream = (residual_entry_input.astype(jnp.float32) + mixed_rows).astype(jnp.bfloat16)
    stream_wide = lax.optimization_barrier(stream).astype(jnp.float32)
    normed_rows = (stream_wide * lax.rsqrt(lax.optimization_barrier(jnp.mean(stream_wide * stream_wide, axis=-1, keepdims=True)) + eps) * feedforward_norm_gain[None, :]).astype(jnp.bfloat16)
    padded = jnp.concatenate([jnp.zeros((2, D), jnp.bfloat16), normed_rows], axis=0)
    row_block = min(token_count, 4096)
    pieces = []
    for offset in range(0, token_count, row_block):
        window = padded[offset:offset + row_block + 2]
        up_gate = jnp.dot(window, gate_up_weight, preferred_element_type=jnp.float32)
        up_value = jnp.dot(window, value_up_weight, preferred_element_type=jnp.float32)
        conv_g = gate_filter_taps[0][None, :] * up_gate[:-2] + gate_filter_taps[1][None, :] * up_gate[1:-1] + gate_filter_taps[2][None, :] * up_gate[2:]
        conv_v = value_filter_taps[0][None, :] * up_value[:-2] + value_filter_taps[1][None, :] * up_value[1:-1] + value_filter_taps[2][None, :] * up_value[2:]
        hidden = (jax.nn.silu(conv_g) * conv_v).astype(jnp.bfloat16)
        running_sum = jnp.zeros((row_block, D), jnp.float32)
        for member in range(N_TP):
            lower = member * FF_DEV
            partial_value = jnp.dot(hidden[:, lower:lower + FF_DEV], down_projection_weight[lower:lower + FF_DEV], preferred_element_type=jnp.float32).astype(jnp.bfloat16)
            running_sum = running_sum + lax.optimization_barrier(partial_value).astype(jnp.float32)
        pieces.append((stream_wide[offset:offset + row_block] + running_sum).astype(jnp.bfloat16))
    return jnp.concatenate(pieces, axis=0)
```

```python
import jax
import jax.numpy as jnp
from jax import lax
from jax.experimental import pallas as pl
from jax.experimental.pallas import tpu as pltpu
from jax.sharding import PartitionSpec as P


BLOCK = 256
TAIL = 16
eps = 1e-06
neg_large = -1e30


def shifted(x, axis, by):
    count = lax.axis_size(axis)
    pairs = [(i, i + by) for i in range(count) if 0 <= i + by < count]
    return lax.ppermute(x, axis, pairs)


def tie(*trees):
    return lax.optimization_barrier(trees)


def gate_log_values(input_gate_logits, forget_gate_logits, forget_decay_offset):
    input_log_value = 15.0 * jnp.tanh(input_gate_logits / 15.0)
    forget_log_sigmoid = (
        jax.nn.log_sigmoid(15.0 * jnp.tanh(forget_gate_logits / 15.0)) + forget_decay_offset
    )
    return (input_log_value, forget_log_sigmoid)


def thirds(x):
    high = x.astype(jnp.bfloat16).astype(jnp.float32)
    rest = x - high
    middle = rest.astype(jnp.bfloat16).astype(jnp.float32)
    return high, middle, rest - middle


def end_state_kernel(columns, keys, values, packed):
    heads, rows, width = packed.shape
    value_width = rows - TAIL
    line = lax.broadcasted_iota(jnp.int32, (TAIL, width), 0)
    for h in range(heads):
        log_weight = columns[:, h : h + 1]
        top = jnp.max(log_weight, axis=0, keepdims=True)
        total = columns[columns.shape[0] - 1 :, heads + h : heads + h + 1]
        weighted = keys[:, h * width : (h + 1) * width].astype(jnp.float32) * jnp.exp(
            log_weight - top
        )
        memory = lax.dot_general(
            values[:, h * value_width : (h + 1) * value_width],
            weighted.astype(jnp.bfloat16),
            (((0,), (0,)), ((), ())),
            preferred_element_type=jnp.float32,
        )
        packed[h, :value_width, :] = memory.astype(jnp.bfloat16)
        tail = jnp.where(line == 0, jnp.sum(weighted, axis=0, keepdims=True), 0.0)
        for at, part in enumerate(thirds(total) + thirds(total + top)):
            tail = jnp.where(line == at + 1, part, tail)
        packed[h, value_width:, :] = tail.astype(jnp.bfloat16)


def output_kernel(
    columns, row_logs, queries, keys, values, prior_memory, prior_normer, gain, gate_logits, out
):
    heads, value_width, width = prior_memory.shape
    count = queries.shape[0]
    block = min(BLOCK, count)
    scale = width ** (-0.5)
    for h in range(heads):
        key_at = slice(h * width, (h + 1) * width)
        value_at = slice(h * value_width, (h + 1) * value_width)
        for start in range(0, count, block):
            stop = start + block
            query = queries[start:stop, key_at]
            stable = columns[start:stop, h : h + 1]
            cumulative = columns[start:stop, heads + h : heads + h + 1]
            prior_log = columns[start:stop, 2 * heads + h : 2 * heads + h + 1]
            raw = (
                lax.dot_general(
                    query,
                    keys[:stop, key_at],
                    (((1,), (1,)), ((), ())),
                    preferred_element_type=jnp.float32,
                )
                * scale
            )
            logits = row_logs[h : h + 1, :stop] - stable
            at = lax.broadcasted_iota(jnp.int32, logits.shape, 0) + start
            source = lax.broadcasted_iota(jnp.int32, logits.shape, 1)
            scores = raw * jnp.exp(jnp.where(source <= at, logits, neg_large))
            numerator = jnp.dot(
                scores.astype(jnp.bfloat16),
                values[:stop, value_at],
                preferred_element_type=jnp.float32,
            )
            denominator = jnp.sum(scores, axis=1, keepdims=True)
            scaled = query.astype(jnp.float32) * scale
            prior_weight = jnp.exp(prior_log - stable)
            numerator = numerator + prior_weight * lax.dot_general(
                scaled,
                prior_memory[h],
                (((1,), (1,)), ((), ())),
                preferred_element_type=jnp.float32,
                precision=lax.Precision.HIGHEST,
            )
            denominator = denominator + prior_weight * jnp.sum(
                scaled * prior_normer[h], axis=1, keepdims=True
            )
            memory_out = numerator / jnp.maximum(
                jnp.abs(denominator), jnp.exp(-(cumulative + stable))
            )
            normed = (
                memory_out
                * lax.rsqrt(jnp.mean(memory_out * memory_out, axis=-1, keepdims=True) + eps)
                * gain[h : h + 1, :]
            )
            gate = jax.nn.sigmoid(gate_logits[start:stop, value_at].astype(jnp.float32))
            out[start:stop, value_at] = (normed * gate).astype(jnp.bfloat16)


def kernel_call(body, shape, **options):
    return pl.pallas_call(
        body,
        out_shape=shape,
        compiler_params=pltpu.CompilerParams(vmem_limit_bytes=48 * 1024 * 1024),
        **options,
    )


class Spread:
    def __init__(self, axis):
        self.axis = axis
        self.count = lax.axis_size(axis)
        self.inner = 2 if self.count % 2 == 0 else 1
        self.outer = self.count // self.inner
        me = lax.axis_index(axis)
        self.at_inner = me % self.inner
        self.at_outer = me // self.inner

    def ring(self, x, by):
        pairs = [
            (o * self.inner + i, (o + by) % self.outer * self.inner + i)
            for o in range(self.outer)
            for i in range(self.inner)
        ]
        return lax.ppermute(x, self.axis, pairs)

    def pair(self, x):
        return lax.ppermute(x, self.axis, [(i, i ^ 1) for i in range(self.count)])

    def ring_steps(self, x, along):
        right, left = x, x
        half = x.shape[along] // 2
        for step in range(1, self.outer // 2 + 1):
            if 2 * step == self.outer:
                low = lax.slice_in_dim(right, 0, half, axis=along)
                high = lax.slice_in_dim(left, half, x.shape[along], axis=along)
                source = (self.at_outer + step) % self.outer
                yield [
                    (self.ring(low, 1), source, 0),
                    (self.ring(high, -1), source, half),
                ]
            else:
                right, left = self.ring(right, 1), self.ring(left, -1)
                yield [
                    (right, (self.at_outer - step) % self.outer, 0),
                    (left, (self.at_outer + step) % self.outer, 0),
                ]


def gather_outer_first(spread, shard, dimension):
    size = shard.shape[dimension]
    other = 1 - dimension
    groups = [[(shard, spread.at_outer, 0)]]
    groups += list(spread.ring_steps(shard, other))
    near, far = [], []
    for group in groups:
        near.append([])
        for piece, source, offset in group:
            own = (source * spread.inner + spread.at_inner) * size
            near[-1].append((piece, own, offset))
            if spread.inner == 2:
                mate = (source * 2 + 1 - spread.at_inner) * size
                far.append((spread.pair(piece), mate, offset))
    return near, far


def gather_inner_first(spread, shard, dimension):
    size = shard.shape[dimension]
    other = 1 - dimension
    mine = [(shard, spread.at_inner)]
    if spread.inner == 2:
        mine.append((spread.pair(shard), 1 - spread.at_inner))
    first = [(piece, (spread.at_outer * spread.inner + i) * size, 0) for piece, i in mine]
    steps = [spread.ring_steps(piece, other) for piece, _ in mine]
    groups = [first]
    for step_groups in zip(*steps):
        groups.append([])
        for group, (_, i) in zip(step_groups, mine):
            for piece, source, offset in group:
                groups[-1].append((piece, (source * spread.inner + i) * size, offset))
    return groups


def assemble(shape, dimension, pieces):
    whole = jnp.zeros(shape, pieces[0][0].dtype)
    for piece, at, offset in pieces:
        where = (at, offset) if dimension == 0 else (offset, at)
        whole = lax.dynamic_update_slice(whole, piece, where)
    return whole


def local(
    residual_entry_input,
    query_matrix_rows,
    key_matrix_rows,
    value_matrix_rows,
    output_gate_logits,
    input_gate_logits,
    forget_gate_logits,
    forget_decay_offset,
    head_norm_gain,
    cell_output_weight,
    feedforward_norm_gain,
    gate_up_weight,
    value_up_weight,
    gate_filter_taps,
    value_filter_taps,
    down_projection_weight,
):
    token_count = query_matrix_rows.shape[0]
    head_count = input_gate_logits.shape[1]
    key_width = query_matrix_rows.shape[1] // head_count
    value_width = value_matrix_rows.shape[1] // head_count
    sp_count = lax.axis_size("sp")
    spread = Spread("sp")

    gate_near, gate_far = gather_outer_first(spread, gate_up_weight, 0)
    value_groups = gather_inner_first(spread, value_up_weight, 0)
    down_near, down_far = gather_outer_first(spread, down_projection_weight, 1)

    input_log_value, forget_log_sigmoid = gate_log_values(
        input_gate_logits.T, forget_gate_logits.T, forget_decay_offset.T
    )
    cumulative = jnp.cumsum(forget_log_sigmoid, axis=1)
    row_logs = input_log_value - cumulative
    local_top = lax.cummax(row_logs, axis=1)

    packed = kernel_call(
        end_state_kernel,
        jax.ShapeDtypeStruct((head_count, value_width + TAIL, key_width), jnp.bfloat16),
    )(
        jnp.concatenate([row_logs, cumulative], axis=0).T,
        key_matrix_rows,
        value_matrix_rows,
    )
    everything = lax.all_gather(packed, "sp")
    position = lax.axis_index("sp")
    marks = everything[:, :, value_width + 1 : value_width + 7, 0].astype(jnp.float32)
    total = marks[:, :, 0] + marks[:, :, 1] + marks[:, :, 2]
    running = marks[:, :, 3] + marks[:, :, 4] + marks[:, :, 5]
    place = jnp.arange(sp_count)
    reached = (place < position)[:, None]
    between = (place[:, None] < place[None, :]) & (place[None, :] < position)
    after = jnp.sum(jnp.where(between[:, :, None], total[None, :, :], 0.0), axis=1)
    logs = jnp.where(reached, after + running, neg_large)
    prior_running = jnp.max(logs, axis=0)
    weights = jnp.where(reached, jnp.exp(logs - prior_running[None, :]), 0.0)
    prior = jnp.sum(
        weights[:, :, None, None]
        * everything[:, :, : value_width + 8, :].astype(jnp.float32),
        axis=0,
    )
    prior_memory = prior[:, :value_width]
    prior_normer = prior[:, value_width : value_width + 1]
    stable = jnp.maximum(local_top, prior_running[:, None])
    columns = jnp.concatenate(
        [stable, cumulative, jnp.broadcast_to(prior_running[:, None], stable.shape)], axis=0
    ).T
    columns, gate_near[1], value_groups[0] = tie(columns, gate_near[1], value_groups[0])

    gated_rows = kernel_call(
        output_kernel,
        jax.ShapeDtypeStruct((token_count, head_count * value_width), jnp.bfloat16),
    )(
        columns,
        row_logs,
        query_matrix_rows,
        key_matrix_rows,
        value_matrix_rows,
        prior_memory,
        prior_normer,
        head_norm_gain,
        output_gate_logits,
    )
    whole_out = lax.all_gather(cell_output_weight, "tp", axis=0, tiled=True)
    gated_rows, down_near[1] = tie(gated_rows, down_near[1])
    own_rows = lax.all_to_all(gated_rows, "tp", split_axis=0, concat_axis=1, tiled=True)
    own_rows, gate_near, value_groups[1] = tie(own_rows, gate_near, value_groups[1])
    mixed_rows = jnp.dot(own_rows, whole_out, preferred_element_type=jnp.float32)
    stream_wide = residual_entry_input.astype(jnp.float32) + mixed_rows
    stream = stream_wide.astype(jnp.bfloat16)
    stream_wide = lax.optimization_barrier(stream).astype(jnp.float32)
    normed_rows = (
        stream_wide
        * lax.rsqrt(jnp.mean(stream_wide * stream_wide, axis=-1, keepdims=True) + eps)
        * feedforward_norm_gain[None, :]
    ).astype(jnp.bfloat16)
    group_rows = lax.all_gather(normed_rows, "tp", axis=0, tiled=True)
    earlier_rows = shifted(group_rows[-2:], "sp", 1)
    window = jnp.concatenate([earlier_rows, group_rows], axis=0)
    width, hidden_width = window.shape[1], gate_up_weight.shape[1]
    flat = lambda groups: [piece for group in groups for piece in group]
    whole_gate = assemble((width, hidden_width), 0, flat(gate_near) + gate_far)
    whole_value = assemble((width, hidden_width), 0, flat(value_groups))
    up_gate = jnp.dot(window, whole_gate, preferred_element_type=jnp.float32)
    up_value = jnp.dot(window, whole_value, preferred_element_type=jnp.float32)
    conv_g = (
        gate_filter_taps[0][None, :] * up_gate[:-2]
        + gate_filter_taps[1][None, :] * up_gate[1:-1]
        + gate_filter_taps[2][None, :] * up_gate[2:]
    )
    conv_v = (
        value_filter_taps[0][None, :] * up_value[:-2]
        + value_filter_taps[1][None, :] * up_value[1:-1]
        + value_filter_taps[2][None, :] * up_value[2:]
    )
    hidden = (jax.nn.silu(conv_g) * conv_v).astype(jnp.bfloat16)
    whole_down = assemble((hidden_width, width), 1, flat(down_near) + down_far)
    ffn_rows = lax.psum_scatter(
        jnp.dot(hidden, whole_down, preferred_element_type=jnp.float32).astype(jnp.bfloat16),
        "tp",
        scatter_dimension=0,
        tiled=True,
    ).astype(jnp.float32)
    return (stream_wide + ffn_rows).astype(jnp.bfloat16)


def solution(mesh):
    in_specs = (
        P(("sp", "tp"), None),
        P("sp", "tp"),
        P("sp", "tp"),
        P("sp", "tp"),
        P("sp", "tp"),
        P("sp", "tp"),
        P("sp", "tp"),
        P("sp", "tp"),
        P("tp", None),
        P("tp", None),
        P(),
        P("sp", "tp"),
        P("sp", "tp"),
        P(None, "tp"),
        P(None, "tp"),
        P("tp", "sp"),
    )
    out_specs = P(("sp", "tp"), None)
    return jax.shard_map(local, mesh=mesh, in_specs=in_specs, out_specs=out_specs, check_vma=False)
```

```python
import jax
import jax.numpy as jnp
from jax import lax
from jax.experimental import pallas as pl
from jax.experimental.pallas import tpu as pltpu
from jax.sharding import PartitionSpec as P


BLOCK = 256
TAIL = 16
eps = 1e-06
neg_large = -1e30


def shifted(x, axis, by):
    count = lax.axis_size(axis)
    pairs = [(i, i + by) for i in range(count) if 0 <= i + by < count]
    return lax.ppermute(x, axis, pairs)


def tie(*trees):
    leaves, form = jax.tree.flatten(trees)
    held = iter(lax.optimization_barrier([x for x in leaves if not isinstance(x, int)]))
    return jax.tree.unflatten(form, [x if isinstance(x, int) else next(held) for x in leaves])


def gate_log_values(input_gate_logits, forget_gate_logits, forget_decay_offset):
    input_log_value = 15.0 * jnp.tanh(input_gate_logits / 15.0)
    forget_log_sigmoid = (
        jax.nn.log_sigmoid(15.0 * jnp.tanh(forget_gate_logits / 15.0)) + forget_decay_offset
    )
    return (input_log_value, forget_log_sigmoid)


def thirds(x):
    high = x.astype(jnp.bfloat16).astype(jnp.float32)
    rest = x - high
    middle = rest.astype(jnp.bfloat16).astype(jnp.float32)
    return high, middle, rest - middle


def end_state_kernel(columns, keys, values, packed):
    heads, rows, width = packed.shape
    value_width = rows - TAIL
    line = lax.broadcasted_iota(jnp.int32, (TAIL, width), 0)
    for h in range(heads):
        log_weight = columns[:, h : h + 1]
        top = jnp.max(log_weight, axis=0, keepdims=True)
        total = columns[columns.shape[0] - 1 :, heads + h : heads + h + 1]
        weighted = keys[:, h * width : (h + 1) * width].astype(jnp.float32) * jnp.exp(
            log_weight - top
        )
        memory = lax.dot_general(
            values[:, h * value_width : (h + 1) * value_width],
            weighted.astype(jnp.bfloat16),
            (((0,), (0,)), ((), ())),
            preferred_element_type=jnp.float32,
        )
        packed[h, :value_width, :] = memory.astype(jnp.bfloat16)
        tail = jnp.where(line == 0, jnp.sum(weighted, axis=0, keepdims=True), 0.0)
        for at, part in enumerate(thirds(total) + thirds(total + top)):
            tail = jnp.where(line == at + 1, part, tail)
        packed[h, value_width:, :] = tail.astype(jnp.bfloat16)


def output_kernel(
    columns, row_logs, queries, keys, values, prior_memory, prior_normer, gain, gate_logits, out
):
    heads, value_width, width = prior_memory.shape
    count = queries.shape[0]
    block = min(BLOCK, count)
    scale = width ** (-0.5)
    for h in range(heads):
        key_at = slice(h * width, (h + 1) * width)
        value_at = slice(h * value_width, (h + 1) * value_width)
        for start in range(0, count, block):
            stop = start + block
            query = queries[start:stop, key_at]
            stable = columns[start:stop, h : h + 1]
            cumulative = columns[start:stop, heads + h : heads + h + 1]
            prior_log = columns[start:stop, 2 * heads + h : 2 * heads + h + 1]
            raw = (
                lax.dot_general(
                    query,
                    keys[:stop, key_at],
                    (((1,), (1,)), ((), ())),
                    preferred_element_type=jnp.float32,
                )
                * scale
            )
            logits = row_logs[h : h + 1, :stop] - stable
            at = lax.broadcasted_iota(jnp.int32, logits.shape, 0) + start
            source = lax.broadcasted_iota(jnp.int32, logits.shape, 1)
            scores = raw * jnp.exp(jnp.where(source <= at, logits, neg_large))
            numerator = jnp.dot(
                scores.astype(jnp.bfloat16),
                values[:stop, value_at],
                preferred_element_type=jnp.float32,
            )
            denominator = jnp.sum(scores, axis=1, keepdims=True)
            scaled = query.astype(jnp.float32) * scale
            prior_weight = jnp.exp(prior_log - stable)
            numerator = numerator + prior_weight * lax.dot_general(
                scaled,
                prior_memory[h],
                (((1,), (1,)), ((), ())),
                preferred_element_type=jnp.float32,
                precision=lax.Precision.HIGHEST,
            )
            denominator = denominator + prior_weight * jnp.sum(
                scaled * prior_normer[h], axis=1, keepdims=True
            )
            memory_out = numerator / jnp.maximum(
                jnp.abs(denominator), jnp.exp(-(cumulative + stable))
            )
            normed = (
                memory_out
                * lax.rsqrt(jnp.mean(memory_out * memory_out, axis=-1, keepdims=True) + eps)
                * gain[h : h + 1, :]
            )
            gate = jax.nn.sigmoid(gate_logits[start:stop, value_at].astype(jnp.float32))
            out[start:stop, value_at] = (normed * gate).astype(jnp.bfloat16)


def kernel_call(body, shape, **options):
    return pl.pallas_call(
        body,
        out_shape=shape,
        compiler_params=pltpu.CompilerParams(vmem_limit_bytes=48 * 1024 * 1024),
        **options,
    )


class Spread:
    def __init__(self, axis):
        self.axis = axis
        self.count = lax.axis_size(axis)
        self.inner = 2 if self.count % 2 == 0 else 1
        self.outer = self.count // self.inner
        me = lax.axis_index(axis)
        self.at_inner = me % self.inner
        self.at_outer = me // self.inner

    def ring(self, x, by):
        pairs = [
            (o * self.inner + i, (o + by) % self.outer * self.inner + i)
            for o in range(self.outer)
            for i in range(self.inner)
        ]
        return lax.ppermute(x, self.axis, pairs)

    def pair(self, x):
        return lax.ppermute(x, self.axis, [(i, i ^ 1) for i in range(self.count)])

    def ring_steps(self, x, along):
        right, left = x, x
        half = x.shape[along] // 2
        for step in range(1, self.outer // 2 + 1):
            if 2 * step == self.outer:
                low = lax.slice_in_dim(right, 0, half, axis=along)
                high = lax.slice_in_dim(left, half, x.shape[along], axis=along)
                source = step
                yield [
                    (self.ring(low, 1), source, 0),
                    (self.ring(high, -1), source, half),
                ]
            else:
                right, left = self.ring(right, 1), self.ring(left, -1)
                yield [
                    (right, self.outer - step, 0),
                    (left, step, 0),
                ]


def gather_outer_first(spread, shard, dimension):
    groups = [[(shard, 0, 0)]] + list(spread.ring_steps(shard, 1 - dimension))
    near, far = [], []
    for group in groups:
        near.append([(piece, step * spread.inner, offset) for piece, step, offset in group])
        if spread.inner == 2:
            far += [(spread.pair(piece), step * 2 + 1, offset) for piece, step, offset in group]
    return near, far


def gather_inner_first(spread, shard, dimension):
    mine = [shard] + ([spread.pair(shard)] if spread.inner == 2 else [])
    groups = [[(piece, i, 0) for i, piece in enumerate(mine)]]
    for step_groups in zip(*[spread.ring_steps(piece, 1 - dimension) for piece in mine]):
        groups.append(
            [
                (piece, step * spread.inner + i, offset)
                for i, group in enumerate(step_groups)
                for piece, step, offset in group
            ]
        )
    return groups


def assemble(dimension, pieces):
    blocks = {}
    for piece, at, offset in sorted(pieces, key=lambda entry: entry[1:]):
        blocks.setdefault(at, []).append(piece)
    whole = [
        parts[0] if len(parts) == 1 else jnp.concatenate(parts, axis=1 - dimension)
        for _, parts in sorted(blocks.items())
    ]
    return jnp.concatenate(whole, axis=dimension)


def reordered(spread, x, to_own):
    size = x.shape[1] // spread.count
    parts = []
    for at in range(spread.count):
        outer, inner = at // spread.inner, at % spread.inner
        move = spread.at_outer if to_own else spread.outer - spread.at_outer
        swapped = jnp.bitwise_xor(spread.at_inner, inner)
        place = (outer + move) % spread.outer * spread.inner + swapped
        parts.append(lax.dynamic_slice_in_dim(x, place * size, size, axis=1))
    return jnp.concatenate(parts, axis=1)


def local(
    residual_entry_input,
    query_matrix_rows,
    key_matrix_rows,
    value_matrix_rows,
    output_gate_logits,
    input_gate_logits,
    forget_gate_logits,
    forget_decay_offset,
    head_norm_gain,
    cell_output_weight,
    feedforward_norm_gain,
    gate_up_weight,
    value_up_weight,
    gate_filter_taps,
    value_filter_taps,
    down_projection_weight,
):
    token_count = query_matrix_rows.shape[0]
    head_count = input_gate_logits.shape[1]
    key_width = query_matrix_rows.shape[1] // head_count
    value_width = value_matrix_rows.shape[1] // head_count
    sp_count = lax.axis_size("sp")
    spread = Spread("sp")

    gate_near, gate_far = gather_outer_first(spread, gate_up_weight, 0)
    value_groups = gather_inner_first(spread, value_up_weight, 0)
    down_near, down_far = gather_outer_first(spread, down_projection_weight, 1)

    input_log_value, forget_log_sigmoid = gate_log_values(
        input_gate_logits.T, forget_gate_logits.T, forget_decay_offset.T
    )
    cumulative = jnp.cumsum(forget_log_sigmoid, axis=1)
    row_logs = input_log_value - cumulative
    local_top = lax.cummax(row_logs, axis=1)

    packed = kernel_call(
        end_state_kernel,
        jax.ShapeDtypeStruct((head_count, value_width + TAIL, key_width), jnp.bfloat16),
    )(
        jnp.concatenate([row_logs, cumulative], axis=0).T,
        key_matrix_rows,
        value_matrix_rows,
    )
    everything = lax.all_gather(packed, "sp")
    position = lax.axis_index("sp")
    marks = everything[:, :, value_width + 1 : value_width + 7, 0].astype(jnp.float32)
    total = marks[:, :, 0] + marks[:, :, 1] + marks[:, :, 2]
    running = marks[:, :, 3] + marks[:, :, 4] + marks[:, :, 5]
    place = jnp.arange(sp_count)
    reached = (place < position)[:, None]
    between = (place[:, None] < place[None, :]) & (place[None, :] < position)
    after = jnp.sum(jnp.where(between[:, :, None], total[None, :, :], 0.0), axis=1)
    logs = jnp.where(reached, after + running, neg_large)
    prior_running = jnp.max(logs, axis=0)
    weights = jnp.where(reached, jnp.exp(logs - prior_running[None, :]), 0.0)
    prior = jnp.sum(
        weights[:, :, None, None]
        * everything[:, :, : value_width + 8, :].astype(jnp.float32),
        axis=0,
    )
    prior_memory = prior[:, :value_width]
    prior_normer = prior[:, value_width : value_width + 1]
    stable = jnp.maximum(local_top, prior_running[:, None])
    columns = jnp.concatenate(
        [stable, cumulative, jnp.broadcast_to(prior_running[:, None], stable.shape)], axis=0
    ).T
    columns, gate_near[1], value_groups[0] = tie(columns, gate_near[1], value_groups[0])

    gated_rows = kernel_call(
        output_kernel,
        jax.ShapeDtypeStruct((token_count, head_count * value_width), jnp.bfloat16),
    )(
        columns,
        row_logs,
        query_matrix_rows,
        key_matrix_rows,
        value_matrix_rows,
        prior_memory,
        prior_normer,
        head_norm_gain,
        output_gate_logits,
    )
    whole_out = lax.all_gather(cell_output_weight, "tp", axis=0, tiled=True)
    gated_rows, down_near[1] = tie(gated_rows, down_near[1])
    own_rows = lax.all_to_all(gated_rows, "tp", split_axis=0, concat_axis=1, tiled=True)
    own_rows, gate_near, value_groups[1] = tie(own_rows, gate_near, value_groups[1])
    mixed_rows = jnp.dot(own_rows, whole_out, preferred_element_type=jnp.float32)
    stream_wide = residual_entry_input.astype(jnp.float32) + mixed_rows
    stream = stream_wide.astype(jnp.bfloat16)
    stream_wide = lax.optimization_barrier(stream).astype(jnp.float32)
    normed_rows = (
        stream_wide
        * lax.rsqrt(jnp.mean(stream_wide * stream_wide, axis=-1, keepdims=True) + eps)
        * feedforward_norm_gain[None, :]
    ).astype(jnp.bfloat16)
    group_rows = lax.all_gather(
        reordered(spread, normed_rows, True), "tp", axis=0, tiled=True
    )
    earlier_rows = shifted(reordered(spread, group_rows[-2:], False), "sp", 1)
    earlier_rows = reordered(spread, earlier_rows, True)
    window = jnp.concatenate([earlier_rows, group_rows], axis=0)
    flat = lambda groups: [piece for group in groups for piece in group]
    whole_gate = assemble(0, flat(gate_near) + gate_far)
    whole_value = assemble(0, flat(value_groups))
    up_gate = jnp.dot(window, whole_gate, preferred_element_type=jnp.float32)
    up_value = jnp.dot(window, whole_value, preferred_element_type=jnp.float32)
    conv_g = (
        gate_filter_taps[0][None, :] * up_gate[:-2]
        + gate_filter_taps[1][None, :] * up_gate[1:-1]
        + gate_filter_taps[2][None, :] * up_gate[2:]
    )
    conv_v = (
        value_filter_taps[0][None, :] * up_value[:-2]
        + value_filter_taps[1][None, :] * up_value[1:-1]
        + value_filter_taps[2][None, :] * up_value[2:]
    )
    hidden = (jax.nn.silu(conv_g) * conv_v).astype(jnp.bfloat16)
    whole_down = assemble(1, flat(down_near) + down_far)
    ffn_rows = lax.psum_scatter(
        jnp.dot(hidden, whole_down, preferred_element_type=jnp.float32).astype(jnp.bfloat16),
        "tp",
        scatter_dimension=0,
        tiled=True,
    )
    ffn_rows = reordered(spread, ffn_rows, False).astype(jnp.float32)
    return (stream_wide + ffn_rows).astype(jnp.bfloat16)


def solution(mesh):
    in_specs = (
        P(("sp", "tp"), None),
        P("sp", "tp"),
        P("sp", "tp"),
        P("sp", "tp"),
        P("sp", "tp"),
        P("sp", "tp"),
        P("sp", "tp"),
        P("sp", "tp"),
        P("tp", None),
        P("tp", None),
        P(),
        P("sp", "tp"),
        P("sp", "tp"),
        P(None, "tp"),
        P(None, "tp"),
        P("tp", "sp"),
    )
    out_specs = P(("sp", "tp"), None)
    return jax.shard_map(local, mesh=mesh, in_specs=in_specs, out_specs=out_specs, check_vma=False)
```
